32 devices in a mesh: sp: 4 (over z), fs: 4 (over y, x), tp: 2 (over core).
Axes of the slice: x: 2, y: 2, z: 4, core: 2. Of those that a mesh axis runs over, the one named last changes fastest.
Arguments:
- tokens: bfloat16 [4, 1024, 2048], P('fs', ('sp', 'tp')), may hold values from -6 to 6
- h_gain: float32 [2048], replicated, may hold values from 0.1 to 1.9
- w_qlat: bfloat16 [2048, 768], P(('sp', 'fs')), may hold values from -0.125 to 0.125
- w_kvlat: bfloat16 [2048, 512], P(('sp', 'fs')), may hold values from -0.125 to 0.125
- w_krope: bfloat16 [2048, 32], P(('sp', 'fs')), may hold values from -0.125 to 0.125
- q_gain: float32 [768], replicated, may hold values from 0.3 to 4.5, as said below
- kv_gain: float32 [512], replicated, may hold values from 0.3 to 4.5, as said below
- w_uq: bfloat16 [768, 1536], P(None, 'tp'), may hold values from -0.375 to 0.375
- w_uk: bfloat16 [512, 1024], P(None, 'tp'), may hold values from -0.4375 to 0.4375
- w_uv: bfloat16 [512, 1024], P(None, 'tp'), may hold values from -0.25 to 0.25
- w_convb: bfloat16 [2048, 1024], P(None, 'tp'), may hold values from -0.125 to 0.125
- w_convc: bfloat16 [2048, 1024], P(None, 'tp'), may hold values from -0.125 to 0.125
- w_convx: bfloat16 [2048, 1024], P(None, 'tp'), may hold values from -0.125 to 0.125
- conv_taps: float32 [3, 1024], P(None, 'tp'), may hold values from -3 to 3
- w_out_attn: bfloat16 [1024, 2048], P('tp'), may hold values from -0.125 to 0.125
- w_out_conv: bfloat16 [1024, 2048], P('tp'), may hold values from -0.125 to 0.125
Outputs:
- mixed: bfloat16 [4, 1024, 2048], P('fs', ('sp', 'tp'))
The draws below stay inside these ranges and needn't reach their ends.
Inputs may be any that keep to these rules, and one draw needn't show every extreme that they name: `q_gain`: positive gains of the query latent's norm. `kv_gain`: positive gains of the key-value latent's norm.
All inputs are finite; a program needn't handle non-finite values.
Results may differ from the reference program's by a relative error of at most 0.017.
The reference program's roundings to bfloat16 on the way count: a program that leaves them out, or rounds other values in their place, can miss the bound.
Values may be sent and summed in bfloat16 or wider, within the bound.
No kernel may reach another device: no remote copies, remote signals or barrier semaphores. Data moves between devices by JAX's collectives and lax.ppermute only.
A program may use at most 64 MiB of HBM per device.

```python
import jax
import jax.numpy as jnp
from jax import lax

D = 2048
H = 16
QR = 768
KVR = 512
NOPE = 64
ROPE = 32
VH = 64
CW = 1024
KW = 3
TOK_DEV = 256
SEQ = 1024
SEQS = 4
N_TP = 2


def draw_q_gain(key, part):
    key = jax.random.fold_in(key, 11)
    return jnp.clip(1.0 + 0.18 * jax.random.normal(key, (QR,), jnp.float32), 0.3, 1.9)


def draw_kv_gain(key, part):
    key = jax.random.fold_in(key, 23)
    return jnp.clip(1.0 + 0.18 * jax.random.normal(key, (KVR,), jnp.float32), 0.3, 1.9)


def block_levels(key, extent, shards, smallest, high):
    level = 1.0
    for dim, parts in shards:
        steps = jax.random.uniform(jax.random.fold_in(jax.random.fold_in(key, 6), dim), (parts,), jnp.float32, smallest / len(shards), high / len(shards))
        level = level * jnp.repeat(jnp.exp(steps), extent[dim] // parts).reshape((-1,) + (1,) * (len(extent) - 1 - dim))
    return level


def normal_values(own_key, shape, deviation, reach, cuts=(), kind=jnp.bfloat16):
    array = jax.random.normal(own_key, shape, jnp.float32) * deviation
    if len(cuts) > 0:
        array = block_levels(own_key, shape, cuts, -0.22, 0.18) * array
    return jnp.clip(array, min=-reach, max=reach).astype(kind)


def setup_inputs(seed: int = 0) -> dict:
    key_list = jax.random.split(jax.random.key(seed), 17)
    tokens = normal_values(key_list[0], (SEQS, SEQ, D), 1.0, 6.0, ((0, 4), (1, 8)))
    h_gain = jnp.clip(1.0 + 0.18 * jax.random.normal(key_list[1], (D,), jnp.float32), 0.1, 1.9)
    w_qlat = normal_values(key_list[2], (D, QR), D ** -0.5, 0.125, ((0, 16),))
    w_kvlat = normal_values(key_list[3], (D, KVR), D ** -0.5, 0.125, ((0, 16),))
    w_krope = normal_values(key_list[4], (D, ROPE), D ** -0.5, 0.125, ((0, 16),))
    q_gain = draw_q_gain(jax.random.fold_in(key_list[16], 71), 0)
    kv_gain = draw_kv_gain(jax.random.fold_in(key_list[16], 71), 0)
    w_uq = normal_values(key_list[7], (QR, H * (NOPE + ROPE)), (QR // 3) ** -0.5, 0.375, ((1, 2),))
    w_uk = normal_values(key_list[8], (KVR, H * NOPE), (KVR // 3) ** -0.5, 0.4375, ((1, 2),))
    w_uv = normal_values(key_list[9], (KVR, H * VH), KVR ** -0.5, 0.25, ((1, 2),))
    w_convb = normal_values(key_list[10], (D, CW), D ** -0.5, 0.125, ((1, 2),))
    w_convc = normal_values(key_list[11], (D, CW), D ** -0.5, 0.125, ((1, 2),))
    w_convx = normal_values(key_list[12], (D, CW), D ** -0.5, 0.125, ((1, 2),))
    conv_taps = normal_values(key_list[13], (KW, CW), 0.58, 3.0, ((1, 2),), jnp.float32)
    w_out_attn = normal_values(key_list[14], (H * VH, D), (H * VH + CW) ** -0.5, 0.125, ((0, 2),))
    w_out_conv = normal_values(key_list[15], (CW, D), (H * VH + CW) ** -0.5, 0.125, ((0, 2),))
    return dict(tokens=tokens, h_gain=h_gain, w_qlat=w_qlat, w_kvlat=w_kvlat, w_krope=w_krope, q_gain=q_gain, kv_gain=kv_gain, w_uq=w_uq, w_uk=w_uk, w_uv=w_uv, w_convb=w_convb, w_convc=w_convc, w_convx=w_convx, conv_taps=conv_taps, w_out_attn=w_out_attn, w_out_conv=w_out_conv)


EPS = 1e-06
THETA = 10000.0

def normalize(values_in, gain):
    return values_in * lax.rsqrt(lax.optimization_barrier(jnp.mean(values_in * values_in, axis=-1, keepdims=True)) + EPS) * gain.astype(jnp.float32)

def angle_table(positions, dims):
    inverse = THETA ** (-jnp.arange(0, dims, 2, dtype=jnp.float32) / dims)
    return positions[:, None] * inverse

def rotate(values_in, angles):
    lower_half, upper_half = jnp.split(values_in, 2, axis=-1)
    cosine = jnp.cos(angles)
    sine_part = jnp.sin(angles)
    return jnp.concatenate([lower_half * cosine - upper_half * sine_part, lower_half * sine_part + upper_half * cosine], axis=-1)

def reference(tokens, h_gain, w_qlat, w_kvlat, w_krope, q_gain, kv_gain, w_uq, w_uk, w_uv, w_convb, w_convc, w_convx, conv_taps, w_out_attn, w_out_conv):
    score_scale = (NOPE + ROPE) ** (-0.5)
    blocks = SEQ // TOK_DEV
    head_width = H * VH // N_TP
    chan_width = CW // N_TP

    def one_sequence(rows_in):
        hidden = normalize(rows_in.astype(jnp.float32), h_gain).astype(jnp.bfloat16)
        query_norm = normalize(jnp.dot(hidden, w_qlat, preferred_element_type=jnp.float32), q_gain).astype(jnp.bfloat16)
        kv_norm = normalize(jnp.dot(hidden, w_kvlat, preferred_element_type=jnp.float32), kv_gain).astype(jnp.bfloat16)
        angles = angle_table(jnp.arange(SEQ, dtype=jnp.float32), ROPE)
        rope_key = rotate(jnp.dot(hidden, w_krope, preferred_element_type=jnp.float32), angles).astype(jnp.bfloat16)
        query = jnp.dot(query_norm, w_uq, preferred_element_type=jnp.float32).reshape(SEQ, H, NOPE + ROPE)
        query = jnp.concatenate([query[..., :NOPE], rotate(query[..., NOPE:], angles[:, None, :])], axis=-1).astype(jnp.bfloat16)
        key_nope = jnp.dot(kv_norm, w_uk, preferred_element_type=jnp.float32).astype(jnp.bfloat16).reshape(SEQ, H, NOPE)
        values = jnp.dot(kv_norm, w_uv, preferred_element_type=jnp.float32).astype(jnp.bfloat16).reshape(SEQ, H, VH)
        keys = jnp.concatenate([key_nope, jnp.broadcast_to(rope_key[:, None, :], (SEQ, H, ROPE))], axis=-1)

        def one_head(arrays):
            query_head, key_head, value_head = arrays

            def one_block(index):
                query_block = lax.dynamic_slice_in_dim(query_head, index * TOK_DEV, TOK_DEV, 0)
                scores = jnp.dot(query_block, key_head.T, preferred_element_type=jnp.float32) * score_scale
                query_pos = index * TOK_DEV + jnp.arange(TOK_DEV, dtype=jnp.int32)
                key_pos = jnp.arange(SEQ, dtype=jnp.int32)
                scores = jnp.where(key_pos[None, :] <= query_pos[:, None], scores, -jnp.inf)
                largest = lax.optimization_barrier(jnp.max(scores, axis=-1, keepdims=True))
                weights = jnp.exp(scores - largest)
                totals = lax.optimization_barrier(jnp.sum(weights, axis=-1, keepdims=True))
                return jnp.dot(weights.astype(jnp.bfloat16), value_head, preferred_element_type=jnp.float32) / totals
            return lax.map(one_block, jnp.arange(blocks, dtype=jnp.int32)).reshape(SEQ, VH)
        attn = lax.map(one_head, (query.transpose(1, 0, 2), keys.transpose(1, 0, 2), values.transpose(1, 0, 2)))
        attn = attn.transpose(1, 0, 2).reshape(SEQ, H * VH).astype(jnp.bfloat16)
        conv_b = jnp.dot(hidden, w_convb, preferred_element_type=jnp.float32)
        conv_c = jnp.dot(hidden, w_convc, preferred_element_type=jnp.float32)
        conv_x = jnp.dot(hidden, w_convx, preferred_element_type=jnp.float32)
        conv_in = (conv_c * conv_x).astype(jnp.bfloat16)
        padded = jnp.concatenate([jnp.zeros((KW - 1, CW), jnp.float32), conv_in.astype(jnp.float32)], axis=0)
        filtered = jnp.zeros((SEQ, CW), jnp.float32)
        for tap in range(KW):
            filtered = filtered + conv_taps[tap].astype(jnp.float32) * padded[tap:tap + SEQ]
        conv_out = (conv_b * filtered).astype(jnp.bfloat16)

        def add_group(summed, group):
            attn_part = lax.dynamic_slice_in_dim(attn, group * head_width, head_width, 1)
            attn_rows = lax.dynamic_slice_in_dim(w_out_attn, group * head_width, head_width, 0)
            conv_part = lax.dynamic_slice_in_dim(conv_out, group * chan_width, chan_width, 1)
            conv_rows = lax.dynamic_slice_in_dim(w_out_conv, group * chan_width, chan_width, 0)
            term = jnp.dot(attn_part, attn_rows, preferred_element_type=jnp.float32) + jnp.dot(conv_part, conv_rows, preferred_element_type=jnp.float32)
            rounded = lax.optimization_barrier(term.astype(jnp.bfloat16))
            return (summed + rounded.astype(jnp.float32), None)
        summed, _ = lax.scan(add_group, jnp.zeros((SEQ, D), jnp.float32), jnp.arange(N_TP, dtype=jnp.int32))
        return summed.astype(jnp.bfloat16)
    return lax.map(one_sequence, tokens)
```

```python
import jax
import jax.numpy as jnp
import numpy as np
from jax import lax
from jax.experimental import pallas as pl
from jax.experimental.pallas import tpu as pltpu
from jax.sharding import PartitionSpec as P

NOPE = 64
ROPE = 32
VH = 64
KW = 3
LANES = 128
EDGE = 8
EPS = 1e-06
THETA = 10000.0
NEG_START = -1e30
LOG2E = 1.4426950408889634
MIB = 1024 * 1024


SMEM_SPEC = pl.BlockSpec(memory_space=pltpu.SMEM)
VMEM_SPEC = pl.BlockSpec(memory_space=pltpu.VMEM)
ANY_SPEC = pl.BlockSpec(memory_space=pl.ANY)


def local_kernel(body, outs, name, limit, in_specs, scratch=(), flops=0, grid=None, out_specs=None):
    return pl.pallas_call(
        body,
        out_shape=tuple(pltpu.VMEM(shape, dtype) for shape, dtype in outs),
        in_specs=in_specs,
        out_specs=tuple(VMEM_SPEC for _ in outs) if out_specs is None else out_specs,
        scratch_shapes=list(scratch),
        compiler_params=pltpu.CompilerParams(vmem_limit_bytes=limit),
        name=name,
        **({} if grid is None else {"grid": grid}),
        cost_estimate=pl.CostEstimate(flops=flops, bytes_accessed=0, transcendentals=0),
    )


def cut_weights(w_qlat, w_kvlat, w_krope):
    rows = w_qlat.shape[0]
    groups = lax.axis_size("tp")
    q_cols = w_qlat.shape[1] // groups
    kv_cols = w_kvlat.shape[1] // groups
    rope_cols = w_krope.shape[1]

    def body(q_ref, kv_ref, rope_ref, kv_out, q_out):
        which = lax.axis_index("tp")
        kv_at = pl.multiple_of(which * kv_cols, LANES)
        q_at = pl.multiple_of(which * q_cols, LANES)
        kv_out[0, :kv_cols, :] = kv_ref[:, pl.ds(kv_at, kv_cols)].T
        kv_out[0, kv_cols:, :] = rope_ref[...]
        q_out[0] = q_ref[:, pl.ds(q_at, q_cols)].T

    return local_kernel(
        body,
        (((1, kv_cols + rope_cols, rows), jnp.bfloat16), ((1, q_cols, rows), jnp.bfloat16)),
        "cut_weights",
        4 * MIB,
        [VMEM_SPEC] * 3,
    )(w_qlat, w_kvlat, w_krope.T)


def stack_parts(parts, name):
    def body(*refs):
        for i, ref in enumerate(refs[:-1]):
            refs[-1][i] = ref[0]

    shape = (len(parts),) + parts[0].shape[1:]
    return local_kernel(body, ((shape, jnp.bfloat16),), name, 4 * MIB, [VMEM_SPEC] * len(parts))(
        *parts
    )[0]


def convolve(own, other, gain, w_b, w_c, w_x, taps):
    each, width = own.shape
    rows = 2 * each
    channels = w_b.shape[1]
    wide = min(2 * LANES, channels)

    def body(own_ref, other_ref, gain_ref, b_ref, c_ref, x_ref, taps_ref, *outs):
        hidden_ref, conv_ref, gate_ref, sum_ref, tail_ref = outs
        which = lax.axis_index("tp")

        @pl.when(pl.program_id(0) == 0)
        def _():
            for ref, place in ((own_ref, which), (other_ref, 1 - which)):
                values = ref[...].astype(jnp.float32)
                scale = lax.rsqrt(jnp.mean(values * values, axis=-1, keepdims=True) + EPS)
                at = pl.multiple_of(place * each, each)
                hidden_ref[pl.ds(at, each), :] = (values * scale * gain_ref[...]).astype(
                    jnp.bfloat16
                )

        hidden = hidden_ref[...]
        gate = jnp.dot(hidden, c_ref[...], preferred_element_type=jnp.float32)
        value = jnp.dot(hidden, x_ref[...], preferred_element_type=jnp.float32)
        out_gate = jnp.dot(hidden, b_ref[...], preferred_element_type=jnp.float32)
        conv_in = (gate * value).astype(jnp.bfloat16).astype(jnp.float32)
        row = lax.broadcasted_iota(jnp.int32, conv_in.shape, 0)
        total = taps_ref[KW - 1 : KW, :] * conv_in
        for back in range(1, KW):
            shifted = jnp.where(row >= back, pltpu.roll(conv_in, back, 0), 0.0)
            total = total + taps_ref[KW - 1 - back : KW - back, :] * shifted
        conv_ref[...] = (out_gate * total).astype(jnp.bfloat16)
        gate_ref[...] = out_gate[:EDGE]
        sum_ref[...] = total[:EDGE]
        tail_ref[...] = conv_in[rows - EDGE :]

    whole = pl.BlockSpec((each, width), lambda j: (0, 0))
    weight = pl.BlockSpec((width, wide), lambda j: (0, j))
    edge = pl.BlockSpec((EDGE, wide), lambda j: (0, j))
    return local_kernel(
        body,
        (
            ((rows, width), jnp.bfloat16),
            ((rows, channels), jnp.bfloat16),
            ((EDGE, channels), jnp.float32),
            ((EDGE, channels), jnp.float32),
            ((EDGE, channels), jnp.float32),
        ),
        "convolve",
        16 * MIB,
        [
            whole,
            whole,
            pl.BlockSpec((1, width), lambda j: (0, 0)),
            weight,
            weight,
            weight,
            pl.BlockSpec((KW, wide), lambda j: (0, j)),
        ],
        flops=6 * rows * width * channels,
        grid=(channels // wide,),
        out_specs=(
            pl.BlockSpec((rows, width), lambda j: (0, 0)),
            pl.BlockSpec((rows, wide), lambda j: (0, j)),
            edge,
            edge,
            edge,
        ),
    )(own, other, gain[None], w_b, w_c, w_x, taps)


def latents(hidden, parts, kept, name):
    rows = hidden.shape[0]
    each, columns, depth = parts[0].shape
    count = each * len(parts)
    rest = columns - kept

    def body(hidden_ref, *refs):
        part_refs, outs = refs[: len(parts)], refs[len(parts) :]
        step, plane, member = lax.axis_index("sp"), lax.axis_index("fs"), lax.axis_index("tp")
        planes = lax.axis_size("fs")
        masks = (0, 1 + member, 2 - member, 3)

        def piece(i):
            block = (step ^ (i % each)) * planes + (plane ^ masks[i // each])
            at = pl.multiple_of(block * depth, depth)
            return hidden_ref[:, pl.ds(at, depth)], part_refs[i // each][i % each]

        total = None
        for i in range(0, count, 2):
            h0, w0 = piece(i)
            h1, w1 = piece(i + 1)
            term = lax.dot_general(
                jnp.concatenate([h0, h1], axis=1),
                jnp.concatenate([w0, w1], axis=1),
                (((1,), (1,)), ((), ())),
                preferred_element_type=jnp.float32,
            )
            total = term if total is None else total + term
        outs[0][...] = total[:, :kept]
        if rest:
            outs[1][...] = total[:, kept:]

    shapes = (((rows, kept), jnp.float32),)
    if rest:
        shapes += (((rows, rest), jnp.float32),)
    return local_kernel(
        body,
        shapes,
        name,
        8 * MIB,
        [VMEM_SPEC] * (1 + len(parts)),
        flops=2 * rows * columns * depth * count,
    )(hidden, *parts)


def finish_keys(latent, rope, tail, gain, table):
    rows, width = latent.shape
    groups = lax.axis_size("tp")
    each = rows // groups
    rope_rows = ROPE * each // width
    per_row = width // each

    def body(latent_ref, rope_ref, tail_ref, gain_ref, table_ref, all_ref, mine_ref, angle, sem):
        at = pl.multiple_of(lax.axis_index("sp") * rows, rows)
        copy = pltpu.make_async_copy(table_ref.at[:, pl.ds(at, rows), :], angle, sem)
        copy.start()
        values = latent_ref[...]
        scale = lax.rsqrt(jnp.mean(values * values, axis=-1, keepdims=True) + EPS)
        normed = values * scale * gain_ref[...]
        half = ROPE // 2
        copy.wait()
        cosine = angle[0][:, NOPE : NOPE + half]
        sine = angle[1][:, NOPE + half : NOPE + ROPE]
        low, high = rope_ref[:, :half], rope_ref[:, half:]
        turned = jnp.concatenate([low * cosine - high * sine, low * sine + high * cosine], axis=1)
        for g in range(groups):
            flat = turned[g * each : (g + 1) * each].T
            packed = jnp.concatenate(
                [flat[i * rope_rows : (i + 1) * rope_rows] for i in range(per_row)], axis=1
            )
            all_ref[g, :each, :] = normed[g * each : (g + 1) * each].astype(jnp.bfloat16)
            all_ref[g, each:, :] = jnp.concatenate([packed, tail_ref[...]], axis=0).astype(
                jnp.bfloat16
            )
        mine_ref[...] = all_ref[lax.axis_index("tp")]

    shape = (each + rope_rows + EDGE, width)
    return local_kernel(
        body,
        (((groups,) + shape, jnp.bfloat16), (shape, jnp.bfloat16)),
        "finish_keys",
        6 * MIB,
        [VMEM_SPEC] * 4 + [ANY_SPEC],
        [pltpu.VMEM((table.shape[0], rows, LANES), jnp.float32), pltpu.SemaphoreType.DMA],
    )(latent, rope, tail, gain[None], table)


def attend(q_latent, q_gain, table, blocks, conv, taps, w_uq, w_uk, w_uv, w_attn, w_conv):
    rows = q_latent.shape[0]
    heads = w_uk.shape[1] // NOPE
    groups, slab, width = blocks[0].shape
    each = rows // groups
    rope_rows = slab - each - EDGE
    per_row = width // each
    count = len(blocks)
    out_width = w_attn.shape[1]
    factor = LOG2E * (NOPE + ROPE) ** (-0.5)
    part = NOPE + ROPE
    heavy = (w_uk, w_uv, w_uq, w_attn, w_conv)

    def body(ql_ref, gain_ref, conv_ref, gate_ref, sum_ref, taps_ref, *refs):
        block_refs = refs[:count]
        refs = refs[count:]
        table_ref, heavy_refs, refs = refs[0], refs[1 : 1 + len(heavy)], refs[1 + len(heavy) :]
        mine_ref, theirs_ref, q_ref, k_ref, v_ref, o_ref, wide_ref, angle = refs[:8]
        uk_ref, uv_ref, uq_ref, wa_ref, wc_ref, sems = refs[8:]
        member, step = lax.axis_index("tp"), lax.axis_index("sp")
        at = pl.multiple_of(step * rows, rows)
        copies = [
            pltpu.make_async_copy(src, dst, sems.at[i])
            for i, (src, dst) in enumerate(
                zip(
                    (*heavy_refs[:3], table_ref.at[:, pl.ds(at, rows), :], *heavy_refs[3:]),
                    (uk_ref, uv_ref, uq_ref, angle, wa_ref, wc_ref),
                )
            )
        ]
        for copy in copies:
            copy.start()
        values = ql_ref[...]
        scale = lax.rsqrt(jnp.mean(values * values, axis=-1, keepdims=True) + EPS)
        q_norm = (values * scale * gain_ref[...]).astype(jnp.bfloat16)
        lane = lax.broadcasted_iota(jnp.int32, (rows, LANES), 1)
        copies[0].wait()
        copies[1].wait()
        for b in range(count):
            kv = jnp.concatenate([block_refs[b][g, :each, :] for g in range(groups)], axis=0)
            pieces = []
            for g in range(groups):
                packed = block_refs[b][g, each : each + rope_rows + EDGE, :].astype(jnp.float32)
                flat = jnp.concatenate(
                    [packed[:rope_rows, i * each : (i + 1) * each] for i in range(per_row)], axis=0
                )
                pieces.append(flat.T)
            rope = jnp.concatenate(pieces, axis=0)
            bias = jnp.where(step >= b, 0.0, NEG_START)
            tail = jnp.concatenate(
                [
                    jnp.zeros((rows, NOPE), jnp.float32),
                    rope,
                    jnp.full((rows, LANES - part), bias, jnp.float32),
                ],
                axis=1,
            )
            key = jnp.dot(kv, uk_ref[...], preferred_element_type=jnp.float32)
            for pair in range(heads // 2):
                two = key[:, pair * LANES : (pair + 1) * LANES]
                k_ref[2 * pair, b] = jnp.where(lane < NOPE, two, tail).astype(jnp.bfloat16)
                k_ref[2 * pair + 1, b] = jnp.where(
                    lane < NOPE, pltpu.roll(two, NOPE, 1), tail
                ).astype(jnp.bfloat16)
            v_ref[b] = jnp.dot(kv, uv_ref[...], preferred_element_type=jnp.float32).astype(
                jnp.bfloat16
            )
        copies[2].wait()
        copies[3].wait()
        wide_ref[:, : heads * part] = jnp.dot(
            q_norm, uq_ref[...], preferred_element_type=jnp.float32
        )
        wide_ref[:, heads * part :] = jnp.zeros((rows, LANES), jnp.float32)
        one_lane = jnp.where(lane == part, 1.0, 0.0)
        for h in range(heads):
            start = h * part // LANES * LANES
            off = h * part - start
            if off:
                raw = pltpu.roll(wide_ref[:, start : start + 2 * LANES], 2 * LANES - off, 1)
                raw = raw[:, :LANES]
            else:
                raw = wide_ref[:, start : start + LANES]
            half = ROPE // 2
            mate = jnp.where(
                lane < NOPE + half, pltpu.roll(raw, LANES - half, 1), pltpu.roll(raw, half, 1)
            )
            q_ref[h] = (raw * angle[0] + mate * angle[1] + one_lane).astype(jnp.bfloat16)
        later = lax.broadcasted_iota(jnp.int32, (rows, rows), 0) >= lax.broadcasted_iota(
            jnp.int32, (rows, rows), 1
        )
        outs = []
        for h in range(heads):
            scores = []
            for b in range(count):
                s = lax.dot_general(
                    q_ref[h],
                    k_ref[h, b],
                    (((1,), (1,)), ((), ())),
                    preferred_element_type=jnp.float32,
                )
                scores.append(jnp.where(later, s, -jnp.inf) if b == 0 else s)
            top = scores[0]
            for s in scores[1:]:
                top = jnp.maximum(top, s)
            top = jnp.max(top, axis=-1, keepdims=True)
            total = jnp.zeros((rows, 1), jnp.float32)
            acc = jnp.zeros((rows, VH), jnp.float32)
            for b in range(count):
                w = jnp.exp2((scores[b] - top) * factor)
                total = total + jnp.sum(w, axis=-1, keepdims=True)
                acc = acc + jnp.dot(
                    w.astype(jnp.bfloat16),
                    v_ref[b, :, h * VH : (h + 1) * VH],
                    preferred_element_type=jnp.float32,
                )
            outs.append(acc / total)
            if h % 2 == 1:
                o_ref[:, (h - 1) * VH : (h + 1) * VH] = jnp.concatenate(outs, axis=1).astype(
                    jnp.bfloat16
                )
                outs = []
        behind = block_refs[1][member, slab - 2 * EDGE :, :].astype(jnp.float32)[EDGE:]
        filled = sum_ref[...]
        row = lax.broadcasted_iota(jnp.int32, filled.shape, 0)
        for back in range(1, KW):
            shifted = jnp.where(row < back, pltpu.roll(behind, back, 0), 0.0)
            filled = filled + taps_ref[KW - 1 - back : KW - back, :] * shifted
        fixed = gate_ref[...] * filled
        first = conv_ref[: 2 * EDGE].astype(jnp.float32)
        conv = jnp.concatenate(
            [
                jnp.concatenate([fixed, first[EDGE:]], axis=0).astype(jnp.bfloat16),
                conv_ref[2 * EDGE :],
            ],
            axis=0,
        )
        copies[4].wait()
        copies[5].wait()
        whole = (
            jnp.dot(o_ref[...], wa_ref[...], preferred_element_type=jnp.float32)
            + jnp.dot(conv, wc_ref[...], preferred_element_type=jnp.float32)
        ).astype(jnp.bfloat16)

        @pl.when(member == 0)
        def _():
            mine_ref[...] = whole[:each]
            theirs_ref[...] = whole[each:]

        @pl.when(member != 0)
        def _():
            mine_ref[...] = whole[each:]
            theirs_ref[...] = whole[:each]

    half = ((each, out_width), jnp.bfloat16)
    return local_kernel(
        body,
        (half, half),
        "attend",
        36 * MIB,
        [VMEM_SPEC] * (6 + count) + [ANY_SPEC] * (1 + len(heavy)),
        [
            pltpu.VMEM((heads, rows, LANES), jnp.bfloat16),
            pltpu.VMEM((heads, count, rows, LANES), jnp.bfloat16),
            pltpu.VMEM((count, rows, heads * VH), jnp.bfloat16),
            pltpu.VMEM((rows, heads * VH), jnp.bfloat16),
            pltpu.VMEM((rows, heads * part + LANES), jnp.float32),
            pltpu.VMEM((table.shape[0], rows, LANES), jnp.float32),
            *[pltpu.VMEM(w.shape, w.dtype) for w in heavy],
            pltpu.SemaphoreType.DMA((len(heavy) + 1,)),
        ],
    )(q_latent, q_gain[None], *conv, taps, *blocks, table, *heavy)


def add_halves(kept, received):
    def body(a_ref, b_ref, out_ref):
        out_ref[...] = (a_ref[...].astype(jnp.float32) + b_ref[...].astype(jnp.float32)).astype(
            jnp.bfloat16
        )

    return pl.pallas_call(
        body,
        out_shape=jax.ShapeDtypeStruct(kept.shape, kept.dtype),
        in_specs=[VMEM_SPEC] * 2,
        out_specs=VMEM_SPEC,
        compiler_params=pltpu.CompilerParams(vmem_limit_bytes=4 * MIB),
        name="add_halves",
    )(kept, received)


def from_behind(array, axis, by):
    size = lax.axis_size(axis)
    pairs = [(i, i + by) for i in range(size) if 0 <= i + by < size]
    return lax.ppermute(array, axis, pairs)


def angle_table(positions, dims):
    inverse = THETA ** (-jnp.arange(0, dims, 2, dtype=jnp.float32) / dims)
    return positions[:, None] * inverse


def turn_table(length):
    inverse = np.float32(THETA) ** (-np.arange(0, ROPE, 2, dtype=np.float32) / np.float32(ROPE))
    angles = np.arange(length, dtype=np.float32)[:, None] * inverse.astype(np.float32)
    cosine, sine = np.cos(angles), np.sin(angles)
    rest = np.zeros((length, LANES - NOPE - ROPE), np.float32)
    keep = np.ones((length, NOPE), np.float32)
    return np.stack(
        [
            np.concatenate([keep, cosine, cosine, rest], axis=1),
            np.concatenate([0 * keep, -sine, sine, rest], axis=1),
        ]
    )


def swap_plane(array, masks):
    n_fs, n_tp = lax.axis_size("fs"), lax.axis_size("tp")
    pairs = [
        (f * n_tp + t, (f ^ masks[t]) * n_tp + t) for f in range(n_fs) for t in range(n_tp)
    ]
    return lax.ppermute(array, ("fs", "tp"), pairs)


def gather_line(array):
    n_sp = lax.axis_size("sp")
    return [array] + [
        lax.ppermute(array, "sp", [(i, i ^ k) for i in range(n_sp)]) for k in range(1, n_sp)
    ]


def gather_plane(line):
    first = swap_plane(line, (1, 2))
    second = swap_plane(line, (2, 1))
    third = swap_plane(first, (2, 1))
    return line, first, second, third


def fast_device(
    tokens,
    h_gain,
    w_qlat,
    w_kvlat,
    w_krope,
    q_gain,
    kv_gain,
    w_uq,
    w_uk,
    w_uv,
    w_convb,
    w_convc,
    w_convx,
    conv_taps,
    w_out_attn,
    w_out_conv,
):
    n_sp, n_tp = lax.axis_size("sp"), lax.axis_size("tp")
    own = tokens[0]
    swap = [(0, 1), (1, 0)]
    table = jnp.asarray(turn_table(n_sp * n_tp * own.shape[0]))
    other = lax.ppermute(own, "tp", swap)
    kv_cut, q_cut = cut_weights(w_qlat, w_kvlat, w_krope)
    kv_line = stack_parts(gather_line(kv_cut), "kv_line")
    q_line = stack_parts(gather_line(q_cut), "q_line")
    kv_parts = gather_plane(kv_line)
    q_parts = gather_plane(q_line)
    hidden, conv_out, gate, summed, tail = convolve(
        own, other, h_gain, w_convb, w_convc, w_convx, conv_taps
    )
    kv_some, rope_latent = latents(hidden, kv_parts, w_kvlat.shape[1] // n_tp, "kv_latent")
    kv_latent = lax.all_gather(kv_some, "tp", axis=1, tiled=True)
    own_block, mine = finish_keys(kv_latent, rope_latent, tail, kv_gain, table)
    blocks = [own_block]
    for k in range(1, n_sp):
        blocks.append(lax.all_gather(from_behind(mine, "sp", k), "tp", axis=0))
    (q_some,) = latents(hidden, q_parts, w_qlat.shape[1] // n_tp, "q_latent")
    q_latent = lax.all_gather(q_some, "tp", axis=1, tiled=True)
    kept, sent = attend(
        q_latent,
        q_gain,
        table,
        blocks,
        (conv_out, gate, summed),
        conv_taps,
        w_uq,
        w_uk,
        w_uv,
        w_out_attn,
        w_out_conv,
    )
    received = lax.ppermute(sent, "tp", swap)
    return add_halves(kept, received)[None]


def normalize(values_in, gain):
    return (
        values_in * lax.rsqrt(jnp.mean(values_in * values_in, axis=-1, keepdims=True) + EPS) * gain
    )


def rotate(values_in, angles):
    lower_half, upper_half = jnp.split(values_in, 2, axis=-1)
    cosine = jnp.cos(angles)
    sine_part = jnp.sin(angles)
    return jnp.concatenate(
        [
            lower_half * cosine - upper_half * sine_part,
            lower_half * sine_part + upper_half * cosine,
        ],
        axis=-1,
    )


def per_device(
    tokens,
    h_gain,
    w_qlat,
    w_kvlat,
    w_krope,
    q_gain,
    kv_gain,
    w_uq,
    w_uk,
    w_uv,
    w_convb,
    w_convc,
    w_convx,
    conv_taps,
    w_out_attn,
    w_out_conv,
):
    own_rows = lax.all_gather(tokens, "tp", axis=1, tiled=True)
    seq_count = own_rows.shape[0]
    rows_here = own_rows.shape[1]
    flat_count = seq_count * rows_here
    hidden = normalize(own_rows.astype(jnp.float32), h_gain).astype(jnp.bfloat16)
    flat_hidden = hidden.reshape(flat_count, hidden.shape[2])
    groups = lax.axis_size("tp")
    member = lax.axis_index("tp")
    q_cols = w_qlat.shape[1] // groups
    kv_cols = w_kvlat.shape[1] // groups
    rope_cols = w_krope.shape[1] // groups
    q_part = lax.dynamic_slice_in_dim(w_qlat, member * q_cols, q_cols, 1)
    kv_part = lax.dynamic_slice_in_dim(w_kvlat, member * kv_cols, kv_cols, 1)
    rope_part = lax.dynamic_slice_in_dim(w_krope, member * rope_cols, rope_cols, 1)
    whole_q, whole_kv, whole_rope = (
        lax.all_gather(q_part, ("sp", "fs"), axis=0, tiled=True),
        lax.all_gather(kv_part, ("sp", "fs"), axis=0, tiled=True),
        lax.all_gather(rope_part, ("sp", "fs"), axis=0, tiled=True),
    )
    partial_latents = (
        jnp.dot(flat_hidden, whole_q, preferred_element_type=jnp.float32),
        jnp.dot(flat_hidden, whole_kv, preferred_element_type=jnp.float32),
        jnp.dot(flat_hidden, whole_rope, preferred_element_type=jnp.float32),
    )
    query_latent, kv_latent, rope_latent = (
        lax.all_gather(partial_latents[0], "tp", axis=1, tiled=True),
        lax.all_gather(partial_latents[1], "tp", axis=1, tiled=True),
        lax.all_gather(partial_latents[2], "tp", axis=1, tiled=True),
    )
    query_latent = query_latent.reshape(seq_count, rows_here, query_latent.shape[1])
    kv_latent = kv_latent.reshape(seq_count, rows_here, kv_latent.shape[1])
    rope_latent = rope_latent.reshape(seq_count, rows_here, rope_latent.shape[1])
    base = lax.axis_index("sp") * rows_here
    query_pos = base + jnp.arange(rows_here, dtype=jnp.int32)
    angles = angle_table(query_pos.astype(jnp.float32), ROPE)
    query_norm = normalize(query_latent, q_gain).astype(jnp.bfloat16)
    kv_norm = normalize(kv_latent, kv_gain).astype(jnp.bfloat16)
    rope_key = rotate(rope_latent, angles[None]).astype(jnp.bfloat16)
    head_count = w_uk.shape[1] // NOPE
    query = jnp.einsum("sqc,cn->sqn", query_norm, w_uq, preferred_element_type=jnp.float32).reshape(
        seq_count, rows_here, head_count, NOPE + ROPE
    )
    query = jnp.concatenate(
        [query[..., :NOPE], rotate(query[..., NOPE:], angles[None, :, None, :])], axis=-1
    ).astype(jnp.bfloat16)
    query = query.transpose(0, 2, 1, 3)
    score_scale = (NOPE + ROPE) ** (-0.5)
    last_query = base + rows_here - 1
    fold_start = (
        jnp.full((seq_count, head_count, rows_here), NEG_START, jnp.float32),
        jnp.zeros((seq_count, head_count, rows_here), jnp.float32),
        jnp.zeros((seq_count, head_count, rows_here, VH), jnp.float32),
    )
    pieces = (
        lax.all_gather(kv_norm, "sp", axis=1, tiled=True),
        lax.all_gather(rope_key, "sp", axis=1, tiled=True),
    )

    def make_keys():
        key_nope = jnp.einsum(
            "skc,cn->skn", pieces[0], w_uk, preferred_element_type=jnp.float32
        ).astype(jnp.bfloat16)
        value_rows = jnp.einsum(
            "skc,cn->skn", pieces[0], w_uv, preferred_element_type=jnp.float32
        ).astype(jnp.bfloat16)
        return (key_nope, value_rows, pieces[1])

    def compute(state):
        running_max, running_sum, weighted = state
        key_nope, value_rows, rope_piece = make_keys()
        width = rope_piece.shape[1]
        keys = jnp.concatenate(
            [
                key_nope.reshape(seq_count, width, head_count, NOPE),
                jnp.broadcast_to(rope_piece[:, :, None, :], (seq_count, width, head_count, ROPE)),
            ],
            axis=-1,
        )
        scores = (
            jnp.einsum("shqd,skhd->shqk", query, keys, preferred_element_type=jnp.float32)
            * score_scale
        )
        key_pos = jnp.arange(width, dtype=jnp.int32)
        visible = key_pos[None, :] <= query_pos[:, None]
        scores = jnp.where(visible[None, None], scores, -jnp.inf)
        new_max = jnp.maximum(running_max, jnp.max(scores, axis=-1))
        weights = jnp.exp(scores - new_max[..., None])
        new_sum = jnp.sum(weights, axis=-1)
        update = jnp.einsum(
            "shqk,skhv->shqv",
            weights.astype(jnp.bfloat16),
            value_rows.reshape(seq_count, width, head_count, VH),
            preferred_element_type=jnp.float32,
        )
        return (new_max, new_sum, update)

    def keep(state):
        return state

    final = lax.cond(jnp.int32(0) <= last_query, compute, keep, fold_start)
    attn = (
        (final[2] / final[1][..., None])
        .transpose(0, 2, 1, 3)
        .reshape(seq_count, rows_here, head_count * VH)
        .astype(jnp.bfloat16)
    )
    conv_b = jnp.dot(flat_hidden, w_convb, preferred_element_type=jnp.float32).reshape(
        seq_count, rows_here, w_convb.shape[1]
    )
    conv_c = jnp.dot(flat_hidden, w_convc, preferred_element_type=jnp.float32)
    conv_x = jnp.dot(flat_hidden, w_convx, preferred_element_type=jnp.float32)
    conv_in = (conv_c * conv_x).astype(jnp.bfloat16).reshape(seq_count, rows_here, w_convc.shape[1])
    edge_rows = from_behind(conv_in[:, rows_here - (KW - 1) :], "sp", 1)
    padded = jnp.concatenate([edge_rows, conv_in], axis=1).astype(jnp.float32)
    filtered = jnp.zeros(conv_b.shape, jnp.float32)
    for tap in range(KW):
        filtered = filtered + conv_taps[tap] * padded[:, tap : tap + rows_here]
    conv_out = (conv_b * filtered).astype(jnp.bfloat16)
    result = lax.psum_scatter(
        (
            jnp.einsum("sqc,cd->qsd", attn, w_out_attn, preferred_element_type=jnp.float32)
            + jnp.einsum("sqc,cd->qsd", conv_out, w_out_conv, preferred_element_type=jnp.float32)
        ).astype(jnp.bfloat16),
        "tp",
        scatter_dimension=0,
        tiled=True,
    )
    return result.transpose(1, 0, 2)


def suits(sizes, args):
    tokens, w_qlat, w_kvlat, w_uk = args[0], args[2], args[3], args[8]
    return (
        sizes["tp"] == 2
        and sizes["fs"] == 4
        and sizes["sp"] > 1
        and sizes["sp"] & (sizes["sp"] - 1) == 0
        and tokens.shape[0] == 1
        and w_qlat.shape[0] % LANES == 0
        and w_qlat.shape[1] % (2 * LANES) == 0
        and w_kvlat.shape[1] % (2 * LANES) == 0
        and tokens.shape[1] % LANES == 0
        and args[10].shape[1] == w_kvlat.shape[1]
        and w_uk.shape[1] % (2 * NOPE) == 0
    )


def solution(mesh):
    in_specs = (
        P("fs", ("sp", "tp"), None),
        P(),
        P(("sp", "fs"), None),
        P(("sp", "fs"), None),
        P(("sp", "fs"), None),
        P(),
        P(),
        P(None, "tp"),
        P(None, "tp"),
        P(None, "tp"),
        P(None, "tp"),
        P(None, "tp"),
        P(None, "tp"),
        P(None, "tp"),
        P("tp", None),
        P("tp", None),
    )
    out_specs = P("fs", ("sp", "tp"), None)
    sizes = mesh.shape

    def either(*args):
        return (fast_device if suits(sizes, args) else per_device)(*args)

    return jax.shard_map(
        either, mesh=mesh, in_specs=in_specs, out_specs=out_specs, check_vma=False
    )
```
